32 devices in a mesh: grp: 2 (over y), ep: 4 (over z), tp: 4 (over x, core).
Axes of the slice: x: 2, y: 2, z: 4, core: 2. Of those that a mesh axis runs over, the one named last changes fastest.
Arguments:
- queries: bfloat16 [1024, 1024], P(('grp', 'ep'), 'tp'), parts along dimension 0, may hold values from -6 to 6
- keys: bfloat16 [1024, 1024], P(('grp', 'ep'), 'tp'), parts along dimension 0, may hold values from -6 to 6
- values: bfloat16 [1024, 1024], P(('grp', 'ep'), 'tp'), parts along dimension 0, may hold values from -6 to 6
- lambdas: float32 [8], P('tp'), may hold values from 0.3 to 0.8
- head_gain: float32 [128], replicated, may hold values from 0.1 to 1.9
- tokens: bfloat16 [2048, 1536], P(('grp', 'ep')), parts along dimension 0, may hold values from -6 to 6
- route_ids: int32 [2048, 2], P(('grp', 'ep')), parts along dimension 0, may hold values from 0 to 3, all different within a row; in each aligned block of 256 rows (0 to 255, 256 to 511, ...) at most 256 rows name the same one
- route_weights: float32 [2048, 2], P(('grp', 'ep')), parts along dimension 0, may hold values from 0.2 to 1
- moe_gain: float32 [1536], replicated, may hold values from 0.1 to 1.9
- w_gate: bfloat16 [4, 1536, 3072], P('ep', None, 'tp'), may hold values from -0.15625 to 0.15625
- w_up: bfloat16 [4, 1536, 3072], P('ep', None, 'tp'), may hold values from -0.15625 to 0.15625
- w_down: bfloat16 [4, 3072, 1536], P('ep', 'tp'), may hold values from -0.109375 to 0.109375
Outputs:
- heads_out: bfloat16 [1024, 1024], P(('grp', 'ep'), 'tp'), parts along dimension 0
- expert_out: bfloat16 [2048, 1536], P(('grp', 'ep'), 'tp'), parts along dimension 0
The draws below stay inside these ranges and needn't reach their ends.
There are 2 independent parts, one for each index of `grp`. The reference program is written for one: setup_inputs(seed, part) draws one part's arguments, and reference() takes and returns one part's arrays. A program takes and returns all parts, laid end to end along the dimension named above; an argument that names none is the same for every part. Nothing has to cross between parts.
Inputs may be any that keep to these rules, and one draw needn't show every extreme that they name: `route_ids`: each row names 2 different experts. In the 256 rows of one device no expert is named more than 256 times, and in every draw some device names some expert exactly 256 times.
All inputs are finite; a program needn't handle non-finite values.
Results may differ from the reference program's by a relative error of at most 0.015.
Values may be sent and summed in bfloat16 or wider, within the bound.
A program may use at most 64 MiB of HBM per device.

```python
import math
import jax
import jax.numpy as jnp
import numpy as np
from jax import lax

D = 1536
FF = 3072
HEADS = 8
HEAD_DIM = 64
VALUE_DIM = 128
TOP = 2
ROW_DEV = 256
EXPERTS = 4
CAP = 256
SEQ = 512
ROWS = 1024
N_EP = 4
N_TP = 4


def draw_pair(key):
    base = jax.random.fold_in(key, 17)
    width = HEADS * 2 * HEAD_DIM
    query_key, key_key = jax.random.split(base, 2)
    query_field = jnp.clip(jax.random.normal(query_key, (SEQ, width), jnp.float32) * 1.33, -6.0, 6.0)
    key_field = jnp.clip(jax.random.normal(key_key, (SEQ, width), jnp.float32) * 1.33, -6.0, 6.0)
    return (query_field, key_field)


def draw_queries(key, part):
    return draw_pair(key)[0].astype(jnp.bfloat16)


def draw_keys(key, part):
    return draw_pair(key)[1].astype(jnp.bfloat16)


def block_scale(own_key, extent, pieces, smallest, largest):
    factor_of = 1.0
    for dim, blocks in pieces:
        heights = jax.random.uniform(jax.random.fold_in(jax.random.fold_in(own_key, 6), dim), (blocks,), jnp.float32, smallest / len(pieces), largest / len(pieces))
        factor_of = factor_of * jnp.repeat(jnp.exp(heights), extent[dim] // blocks).reshape((-1,) + (1,) * (len(extent) - 1 - dim))
    return factor_of


def deal_out(own_key, own, number, rows, amount, top, most, slope):
    ranking = jax.random.permutation(own_key, amount)
    heavy_load, usual = shares(amount, rows * top, most, slope, True), shares(amount, rows * top, most, slope, False)
    places = jnp.arange(amount)

    def named(sizes, offset_by):
        used = int((sizes > 0).sum())
        fixed = max(1, used // 4)
        moved = fixed + (places - fixed + offset_by * (used - fixed)) % max(1, amount - fixed)
        return jnp.zeros((amount,), jnp.int32).at[ranking[jnp.where(places < fixed, places, moved)]].set(jnp.asarray(sizes, jnp.int32))

    sizes = jnp.where(number % 4 == 0, named(heavy_load, number // 4), named(usual, number - number // 4 - 1))
    mixed = jax.random.permutation(jax.random.fold_in(own, 3), amount)
    source_of, sink = mixed[0:amount // 2 * 2:2], mixed[1:amount // 2 * 2:2]
    margin = jnp.minimum(sizes[source_of] - 1, most - sizes[sink]) // 2
    margin = jnp.where((source_of == ranking[0]) | (sink == ranking[0]) | (sizes[sink] == 0), 0, jnp.maximum(margin, 0))
    moved = jax.random.randint(jax.random.fold_in(own, 4), (amount // 2,), 0, 1 << 20) % (margin + 1)
    sizes = sizes.at[source_of].add(-moved).at[sink].add(moved)
    items = jnp.searchsorted(jnp.cumsum(sizes), jnp.arange(rows * top), side="right").astype(jnp.int32)
    listing = items.reshape(top, rows).T
    listing = listing[jax.random.permutation(jax.random.fold_in(own, 1), rows)]
    offset_by = jax.random.randint(jax.random.fold_in(own, 2), (rows, 1), 0, top)
    return jnp.take_along_axis(listing, (jnp.arange(top)[None, :] + offset_by) % top, axis=1)


def shares(count, total, bound, slope, full):
    weights = [(1 << 20) // math.isqrt(rank ** slope) + 1 for rank in range(1, count + 1)]
    largest = bound if full else min(bound, max(-(-total // count), total * weights[0] // sum(weights)))
    least = 1 if total - largest >= count - 1 else 0
    counts, surplus = [largest] + [least] * (count - 1), total - largest - least * (count - 1)
    while surplus > 0:
        free = [i for i in range(1, count) if counts[i] < largest] or [i for i in range(1, count) if counts[i] < bound]
        mass, budget = sum([weights[i] for i in free]), surplus
        for i in free:
            more = min(bound - counts[i], max(1, budget * weights[i] // mass), surplus)
            counts[i] = counts[i] + more
            surplus = surplus - more
    return np.array(counts)


def bell_draw(key, dims, spread, limit, shards=(), kind=jnp.bfloat16):
    factor_of = block_scale(key, dims, shards, -0.22, 0.18) if shards else 1.0
    entries = jax.random.normal(key, dims, jnp.float32) * spread * factor_of
    return jnp.minimum(jnp.maximum(entries, -limit), limit).astype(kind)


def setup_inputs(seed: int = 0, part: int = 0) -> dict:
    splits = jax.random.split(jax.random.key(seed), 13)
    own_keys = jax.random.split(jax.random.fold_in(splits[12], part), 13)
    queries = draw_queries(jax.random.fold_in(jax.random.fold_in(splits[12], part), 71), part)
    keys = draw_keys(jax.random.fold_in(jax.random.fold_in(splits[12], part), 71), part)
    values = bell_draw(own_keys[2], (SEQ, HEADS * VALUE_DIM), 1.0, 6.0, ((0, 4), (1, 4)))
    lambdas = jnp.clip(0.3 + 0.5 * jax.random.uniform(splits[3], (HEADS,), jnp.float32) ** block_scale(splits[3], (HEADS,), ((0, 4),), -0.2, 0.2), 0.3, 0.8)
    head_gain = jnp.clip(1.0 + 0.18 * jax.random.normal(splits[4], (VALUE_DIM,), jnp.float32), 0.1, 1.9)
    tokens = bell_draw(own_keys[5], (ROWS, D), 1.0, 6.0, ((0, 4),))
    route_ids_keys = jax.random.split(jax.random.fold_in(own_keys[6], 1), ROWS // ROW_DEV)
    route_ids_turns = jax.random.permutation(jax.random.fold_in(own_keys[6], 3), ROWS // ROW_DEV)
    route_ids = jax.vmap(lambda own, number: deal_out(jax.random.fold_in(own_keys[6], 2), own, number, ROW_DEV, EXPERTS, TOP, CAP, 2))(route_ids_keys, route_ids_turns).reshape((ROWS, TOP))
    route_weights = jnp.clip(0.2 + 0.8 * jax.random.uniform(own_keys[7], (ROWS, TOP), jnp.float32) ** block_scale(own_keys[7], (ROWS, TOP), ((0, 4),), -0.2, 0.2), 0.2, 1.0)
    moe_gain = jnp.clip(1.0 + 0.18 * jax.random.normal(splits[8], (D,), jnp.float32), 0.1, 1.9)
    w_gate = bell_draw(splits[9], (EXPERTS, D, FF), D ** -0.5, 0.15625, ((0, 4), (2, 4)))
    w_up = bell_draw(splits[10], (EXPERTS, D, FF), D ** -0.5, 0.15625, ((0, 4), (2, 4)))
    w_down = bell_draw(splits[11], (EXPERTS, FF, D), FF ** -0.5, 0.109375, ((0, 4), (1, 4)))
    return dict(queries=queries, keys=keys, values=values, lambdas=lambdas, head_gain=head_gain, tokens=tokens, route_ids=route_ids, route_weights=route_weights, moe_gain=moe_gain, w_gate=w_gate, w_up=w_up, w_down=w_down)


def head_mix(operands):
    query_head, key_head, value_head, lambda_head, head_gain = operands
    block = math.gcd(SEQ, 512)
    query_blocks = query_head.reshape(SEQ // block, block, 2, HEAD_DIM)

    def one_block(query_part):
        results = []
        for component in range(2):
            scores = jnp.dot(query_part[:, component], key_head[:, component].T, preferred_element_type=jnp.float32) * HEAD_DIM ** (-0.5)
            highest = lax.optimization_barrier(jnp.max(scores, axis=1, keepdims=True))
            shifted = jnp.exp(scores - highest)
            totals = lax.optimization_barrier(jnp.sum(shifted, axis=1, keepdims=True))
            sums = jnp.dot(shifted.astype(jnp.bfloat16), value_head, preferred_element_type=jnp.float32)
            results.append(sums / totals)
        mixed = results[0] - lambda_head * results[1]
        scaled = mixed * lax.rsqrt(lax.optimization_barrier(jnp.mean(mixed * mixed, axis=1, keepdims=True)) + 1e-06) * head_gain
        return scaled.astype(jnp.bfloat16)
    return lax.map(one_block, query_blocks).reshape(SEQ, VALUE_DIM)

def reference(queries, keys, values, lambdas, head_gain, tokens, route_ids, route_weights, moe_gain, w_gate, w_up, w_down):
    query_heads = jnp.transpose(queries.reshape(SEQ, HEADS, 2, HEAD_DIM), (1, 0, 2, 3))
    key_heads = jnp.transpose(keys.reshape(SEQ, HEADS, 2, HEAD_DIM), (1, 0, 2, 3))
    value_heads = jnp.transpose(values.reshape(SEQ, HEADS, VALUE_DIM), (1, 0, 2))
    gains = jnp.broadcast_to(head_gain, (HEADS, VALUE_DIM))
    mixed_heads = lax.map(head_mix, (query_heads, key_heads, value_heads, lambdas, gains))
    heads_out = jnp.transpose(mixed_heads, (1, 0, 2)).reshape(SEQ, HEADS * VALUE_DIM)
    token_float = tokens.astype(jnp.float32)
    normed = (token_float * lax.rsqrt(lax.optimization_barrier(jnp.mean(token_float * token_float, axis=1, keepdims=True)) + 1e-06) * moe_gain).astype(jnp.bfloat16)
    flat_ids = route_ids.reshape(N_EP, ROW_DEV * TOP)
    onehot = (flat_ids[:, :, None] == jnp.arange(EXPERTS, dtype=jnp.int32)[None, None, :]).astype(jnp.int32)
    earlier = jnp.cumsum(onehot, axis=1) - onehot
    position = lax.optimization_barrier(jnp.sum(earlier * onehot, axis=2)).astype(jnp.int32)
    source = jnp.broadcast_to(jnp.arange(N_EP, dtype=jnp.int32)[:, None], (N_EP, ROW_DEV * TOP))
    owner_row = source * ROW_DEV + jnp.arange(ROW_DEV * TOP, dtype=jnp.int32)[None, :] // TOP
    table = jnp.full((EXPERTS, N_EP, CAP), ROWS, jnp.int32).at[flat_ids, source, position].set(owner_row)
    padded = jnp.concatenate([normed, jnp.zeros((1, D), jnp.bfloat16)], axis=0)

    def expert_pass(operands):
        rows_index, gate_mat, up_mat, down_mat = operands
        arrived = padded[rows_index.reshape(-1)]
        gate = jnp.dot(arrived, gate_mat, preferred_element_type=jnp.float32)
        upward = jnp.dot(arrived, up_mat, preferred_element_type=jnp.float32)
        hidden = (jax.nn.silu(gate) * upward).astype(jnp.bfloat16)
        hidden_blocks = jnp.transpose(hidden.reshape(-1, N_TP, FF // N_TP), (1, 0, 2)).astype(jnp.float32)
        down_blocks = down_mat.reshape(N_TP, FF // N_TP, D).astype(jnp.float32)
        partial_sums = jnp.einsum('jsf,jfd->jsd', hidden_blocks, down_blocks)
        rounded = lax.optimization_barrier(partial_sums.astype(jnp.bfloat16))
        return lax.optimization_barrier(jnp.sum(rounded.astype(jnp.float32), axis=0)).astype(jnp.bfloat16)
    results = lax.map(expert_pass, (table, w_gate, w_up, w_down)).reshape(EXPERTS, N_EP, CAP, D)
    picked = results[flat_ids, source, position].reshape(ROWS, TOP, D).astype(jnp.float32)
    expert_out = jnp.einsum('rkd,rk->rd', picked, route_weights).astype(jnp.bfloat16)
    return (heads_out, expert_out)
```

```python
import functools

import jax
import jax.numpy as jnp
from jax import lax
from jax.experimental import pallas as pl
from jax.experimental.pallas import tpu as pltpu
from jax.sharding import PartitionSpec as P

MESH = pl.DeviceIdType.MESH
F32 = jnp.float32
BF16 = jnp.bfloat16

def attend(queries, keys, values, lambdas, head_gain):
    row_count = queries.shape[0]
    head_count = lambdas.shape[0]
    head_dim = queries.shape[1] // (2 * head_count)
    value_dim = values.shape[1] // head_count
    query_parts = queries.reshape(row_count, head_count, 2, head_dim)
    score_scale = head_dim ** (-0.5)
    running = jnp.full((head_count, 2, row_count), -1e30, jnp.float32)
    key_piece = lax.all_gather(keys, "ep", axis=0, tiled=True)
    value_piece = lax.all_gather(values, "ep", axis=0, tiled=True)
    count = key_piece.shape[0]
    key_parts = key_piece.reshape(count, head_count, 2, head_dim)
    value_parts = value_piece.reshape(count, head_count, value_dim)
    scores = (
        jnp.einsum("qhcd,khcd->hcqk", query_parts, key_parts, preferred_element_type=jnp.float32)
        * score_scale
    )
    newest = jnp.maximum(running, jnp.max(scores, axis=-1))
    weights_now = jnp.exp(scores - newest[..., None])
    totals = jnp.sum(weights_now, axis=-1)
    sums = jnp.einsum(
        "hcqk,khe->hcqe",
        weights_now.astype(jnp.bfloat16),
        value_parts,
        preferred_element_type=jnp.float32,
    )
    running, totals, sums = (newest, totals, sums)
    means = sums / totals[..., None]
    mixed = means[:, 0] - lambdas[:, None, None] * means[:, 1]
    scaled = mixed * lax.rsqrt(jnp.mean(mixed * mixed, axis=-1, keepdims=True) + 1e-06) * head_gain
    return (
        jnp.transpose(scaled, (1, 0, 2))
        .reshape(row_count, head_count * value_dim)
        .astype(jnp.bfloat16)
    )


def experts(tokens, route_ids, route_weights, moe_gain, w_gate, w_up, w_down):
    row_count, width = tokens.shape
    top_count = route_ids.shape[1]
    ep_size = lax.axis_size("ep")
    tp_size = lax.axis_size("tp")
    expert_count = w_gate.shape[0] * ep_size
    capacity = 2 * row_count * top_count // expert_count
    token_float = tokens.astype(jnp.float32)
    normed = (
        token_float
        * lax.rsqrt(jnp.mean(token_float * token_float, axis=1, keepdims=True) + 1e-06)
        * moe_gain
    ).astype(jnp.bfloat16)
    flat_ids = route_ids.reshape(-1)
    onehot = (flat_ids[:, None] == jnp.arange(expert_count, dtype=jnp.int32)[None, :]).astype(
        jnp.int32
    )
    earlier = jnp.cumsum(onehot, axis=0) - onehot
    position = jnp.sum(earlier * onehot, axis=1)
    slot_index = flat_ids * capacity + position
    owners = (
        jnp.full((expert_count * capacity,), row_count, jnp.int32)
        .at[slot_index]
        .set(jnp.arange(row_count * top_count, dtype=jnp.int32) // top_count)
    )
    padded = jnp.concatenate([normed, jnp.zeros((1, width), jnp.bfloat16)], axis=0)
    outgoing = padded[owners].reshape(expert_count, capacity, width)
    gate_mat = w_gate[0]
    up_mat = w_up[0]
    down_mat = w_down[0]
    slice_width = width // tp_size
    own_columns = lax.dynamic_slice_in_dim(
        outgoing, lax.axis_index("tp") * slice_width, slice_width, 2
    )
    arrived = lax.all_to_all(own_columns, "ep", split_axis=0, concat_axis=0, tiled=True)
    piece = lax.all_gather(arrived, "tp", axis=2, tiled=True)
    gate = jnp.einsum("scd,df->scf", piece, gate_mat, preferred_element_type=jnp.float32)
    upward = jnp.einsum("scd,df->scf", piece, up_mat, preferred_element_type=jnp.float32)
    hidden = (jax.nn.silu(gate) * upward).astype(jnp.bfloat16)
    flat_hidden = hidden.reshape(-1, hidden.shape[2])
    summed = lax.psum_scatter(
        jnp.einsum("fd,sf->ds", down_mat, flat_hidden, preferred_element_type=jnp.float32).astype(
            jnp.bfloat16
        ),
        "tp",
        scatter_dimension=0,
        tiled=True,
    )
    back = lax.all_to_all(summed, "ep", split_axis=1, concat_axis=1, tiled=True)
    picked = (
        jnp.take(back, slot_index, axis=1).astype(jnp.float32).reshape(-1, row_count, top_count)
    )
    combined = jnp.einsum("drk,rk->rd", picked, route_weights)
    return combined.astype(jnp.bfloat16)


def visit_order(n):
    return [sorted((s for s in range(n) if s != e), key=lambda s: (abs(s - e), s)) for e in range(n)]


def fused_kernel(
    n,
    q_ref,
    k_ref,
    v_ref,
    lam_ref,
    hgain_ref,
    tok_ref,
    ids_ref,
    rw_ref,
    mgain_ref,
    wg_hbm,
    wu_hbm,
    wd_hbm,
    heads_ref,
    out_ref,
    wg,
    wu,
    wd,
    gathered,
    kbuf,
    vbuf,
    hid,
    part,
    core_in,
    s_own,
    s_out,
    x_in,
    t_out,
    ret,
    wsem,
    own_send,
    z_send,
    z_recv,
    x_send,
    x_recv,
    c_send,
    c_recv,
    kv_own,
    kv_send,
    kv_recv,
    r1_send,
    r1_recv,
    r2_send,
    r2_recv,
    r3_send,
    r3_recv,
):
    e = lax.axis_index("ep")
    t = lax.axis_index("tp")
    xi = t // 2
    ci = lax.rem(t, 2)
    core_peer = {"tp": 2 * xi + 1 - ci}
    x_peer = {"tp": 2 * (1 - xi) + ci}
    rows, width = tok_ref.shape
    cols = width // 4
    kv_rows = k_ref.shape[0]

    def colblock(j):
        return pl.ds(pl.multiple_of(j * cols, 128), cols)

    def remote(src, dst, ss, rs, dev):
        return pltpu.make_async_remote_copy(
            src_ref=src, dst_ref=dst, send_sem=ss, recv_sem=rs, device_id=dev, device_id_type=MESH
        )

    weights = [
        pltpu.make_async_copy(a, b, wsem.at[i])
        for i, (a, b) in enumerate(((wg_hbm.at[0], wg), (wu_hbm.at[0], wu), (wd_hbm.at[0], wd)))
    ]
    for c in weights:
        c.start()

    barrier = pltpu.get_barrier_semaphore()
    for d in range(1, n):
        pl.semaphore_signal(barrier, inc=1, device_id={"ep": lax.rem(e + d, n)}, device_id_type=MESH)
    pl.semaphore_signal(barrier, inc=1, device_id=core_peer, device_id_type=MESH)
    pl.semaphore_signal(barrier, inc=1, device_id=x_peer, device_id_type=MESH)

    step = 32

    @pl.loop(0, rows // step)
    def _(i):
        sl = pl.ds(pl.multiple_of(i * step, step), step)
        v = tok_ref[sl, :].astype(F32)
        scale = lax.rsqrt(jnp.mean(v * v, axis=1, keepdims=True) + 1e-06)
        gathered[e, sl, :] = (v * scale * mgain_ref[...]).astype(BF16)

    pl.semaphore_wait(barrier, n + 1)

    has_left = e > 0
    has_right = e < n - 1
    sides = ((0, has_left, e - 1), (1, has_right, e + 1))
    own_tok = gathered.at[e, :, colblock(t)]
    own_kv = pl.ds(pl.multiple_of(e * kv_rows, kv_rows), kv_rows)

    def own_copies(side, peer):
        dev = {"ep": peer}
        return (
            remote(own_tok, own_tok, own_send.at[side], z_recv.at[e], dev),
            remote(k_ref, kbuf.at[own_kv], kv_own.at[0, side], kv_recv.at[0, e], dev),
            remote(v_ref, vbuf.at[own_kv], kv_own.at[1, side], kv_recv.at[1, e], dev),
        )

    for side, has, peer in sides:

        @pl.when(has)
        def _():
            for c in own_copies(side, peer):
                c.start()

    kbuf[own_kv, :] = k_ref[...]
    vbuf[own_kv, :] = v_ref[...]

    orders = visit_order(n)

    def nth(k):
        s = jnp.int32(orders[0][k])
        for i in range(1, n):
            s = jnp.where(e == i, jnp.int32(orders[i][k]), s)
        return s

    visits = [nth(k) for k in range(n - 1)]

    def forward_of(s):
        from_left = s < e
        has = jnp.logical_or(
            jnp.logical_and(from_left, has_right),
            jnp.logical_and(jnp.logical_not(from_left), has_left),
        )
        return has, {"ep": jnp.clip(jnp.where(from_left, e + 1, e - 1), 0, n - 1)}

    def z_copy(s):
        blk = gathered.at[s, :, colblock(t)]
        return remote(blk, blk, z_send.at[s], z_recv.at[s], forward_of(s)[1])

    def x_copy(s):
        blk = gathered.at[s, :, colblock(t)]
        return remote(blk, blk, x_send.at[s], x_recv.at[s], x_peer)

    def c_copy(s, which):
        blk = gathered.at[s, :, colblock(t if which == 0 else 2 * (1 - xi) + ci)]
        return remote(blk, blk, c_send.at[which, s], c_recv.at[which, s], core_peer)

    def kv_copy(which, s):
        sl = pl.ds(pl.multiple_of(s * kv_rows, kv_rows), kv_rows)
        blk = (kbuf, vbuf)[which].at[sl]
        return remote(blk, blk, kv_send.at[which, s], kv_recv.at[which, s], forward_of(s)[1])

    def r1_copy(s, xx):
        return remote(
            part.at[s, :, colblock(2 * xx + 1 - ci)],
            core_in.at[s, xx],
            r1_send.at[xx, s],
            r1_recv.at[xx, s],
            core_peer,
        )

    def r2_copy(s):
        return remote(s_out.at[s], x_in.at[s], r2_send.at[s], r2_recv.at[s], x_peer)

    def r3_copy(s):
        return remote(t_out.at[s], ret.at[e], r3_send.at[s], r3_recv.at[e], {"ep": s})

    def ffn(s):
        ff = wg.shape[1]
        nb = 256

        @pl.loop(0, ff // nb)
        def _(b):
            sl = pl.ds(pl.multiple_of(b * nb, nb), nb)
            g = jnp.dot(gathered[s], wg[:, sl], preferred_element_type=F32)
            u = jnp.dot(gathered[s], wu[:, sl], preferred_element_type=F32)
            hid[:, sl] = (g / (1.0 + jnp.exp(-g)) * u).astype(BF16)

        ob = 512

        @pl.loop(0, width // ob)
        def _(b):
            sl = pl.ds(pl.multiple_of(b * ob, ob), ob)
            part[s, :, sl] = jnp.dot(hid[...], wd[:, sl], preferred_element_type=F32).astype(BF16)

        r1_copy(s, 1 - xi).start()
        r1_copy(s, xi).start()

    def reduce_core(s):
        r1_copy(s, 1 - xi).wait_recv()
        far = part[s, :, colblock(2 * (1 - xi) + ci)].astype(F32) + core_in[s, 1 - xi].astype(F32)
        s_out[s] = far.astype(BF16)
        r2_copy(s).start()
        r1_copy(s, xi).wait_recv()
        s_own[s] = part[s, :, colblock(t)].astype(F32) + core_in[s, xi].astype(F32)

    def reduce_x(s):
        r2_copy(s).wait_recv()
        t_out[s] = (s_own[s] + x_in[s].astype(F32)).astype(BF16)

        @pl.when(s != e)
        def _():
            r3_copy(s).start()

    def arrive(s):
        z_copy(s).wait_recv()

        @pl.when(forward_of(s)[0])
        def _():
            z_copy(s).start()

        x_copy(s).start()
        c_copy(s, 0).start()

    def relay_kv(s):
        for w in (0, 1):
            kv_copy(w, s).wait_recv()

            @pl.when(forward_of(s)[0])
            def _():
                kv_copy(w, s).start()

    def attend():
        heads = lam_ref.shape[0]
        vd = v_ref.shape[1] // heads
        hd = q_ref.shape[1] // (2 * heads)
        qr = q_ref.shape[0]
        first = lax.broadcasted_iota(jnp.int32, (qr, 2 * hd), 1) < hd
        for h in range(heads):
            q = q_ref[:, h * 2 * hd : (h + 1) * 2 * hd].astype(F32)
            both = jnp.concatenate(
                [jnp.where(first, q, 0.0).astype(BF16), jnp.where(first, 0.0, q).astype(BF16)], axis=0
            )
            kh = kbuf[:, h * 2 * hd : (h + 1) * 2 * hd]
            vh = vbuf[:, h * vd : (h + 1) * vd]
            scores = lax.dot_general(
                both, kh, (((1,), (1,)), ((), ())), preferred_element_type=F32
            ) * (hd ** (-0.5))
            ex = jnp.exp(scores - jnp.max(scores, axis=1, keepdims=True))
            tot = jnp.sum(ex, axis=1, keepdims=True)
            sums = jnp.dot(ex.astype(BF16), vh, preferred_element_type=F32) / tot
            mixed = sums[:qr] - lam_ref[h] * sums[qr:]
            norm = lax.rsqrt(jnp.mean(mixed * mixed, axis=1, keepdims=True) + 1e-06)
            heads_ref[:, h * vd : (h + 1) * vd] = (mixed * norm * hgain_ref[...]).astype(BF16)

    for c in weights:
        c.wait()
    ffn(e)
    done = e
    waiting = None
    for s in visits:
        arrive(s)
        reduce_core(done)
        x_copy(s).wait_recv()
        c_copy(s, 1).start()
        c_copy(s, 0).wait_recv()
        c_copy(s, 1).wait_recv()
        if waiting is not None:
            reduce_x(waiting)
        ffn(s)
        relay_kv(s)
        waiting, done = done, s
    reduce_core(done)
    reduce_x(waiting)
    attend()
    reduce_x(done)

    total = None
    ids = ids_ref[...]
    rw = rw_ref[...]

    def weight_of(x):
        return jnp.sum(jnp.where(ids == x, rw, 0.0), axis=1, keepdims=True)

    total = t_out[e].astype(F32) * weight_of(e)
    for s in visits:
        remote(t_out.at[s], ret.at[s], r3_send.at[s], r3_recv.at[s], {"ep": s}).wait_recv()
        total = total + ret[s].astype(F32) * weight_of(s)
    out_ref[...] = total.astype(BF16)

    for side, has, peer in sides:

        @pl.when(has)
        def _():
            for c in own_copies(side, peer):
                c.wait_send()

    for s in [e] + visits:
        r1_copy(s, 1 - xi).wait_send()
        r1_copy(s, xi).wait_send()
        r2_copy(s).wait_send()
    for s in visits:
        x_copy(s).wait_send()
        c_copy(s, 0).wait_send()
        c_copy(s, 1).wait_send()
        r3_copy(s).wait_send()

        @pl.when(forward_of(s)[0])
        def _():
            z_copy(s).wait_send()
            kv_copy(0, s).wait_send()
            kv_copy(1, s).wait_send()


def fused(queries, keys, values, lambdas, head_gain, tokens, route_ids, route_weights, moe_gain, w_gate, w_up, w_down):
    n = lax.axis_size("ep")
    rows, width = tokens.shape
    cols = width // 4
    ff = w_gate.shape[2]
    vmem = pl.BlockSpec(memory_space=pltpu.VMEM)
    smem = pl.BlockSpec(memory_space=pltpu.SMEM)
    hbm = pl.BlockSpec(memory_space=pl.ANY)
    dma = pltpu.SemaphoreType.DMA
    return pl.pallas_call(
        functools.partial(fused_kernel, n),
        out_shape=(
            jax.ShapeDtypeStruct((queries.shape[0], values.shape[1]), BF16),
            jax.ShapeDtypeStruct((rows, cols), BF16),
        ),
        in_specs=[vmem, vmem, vmem, smem, vmem, vmem, vmem, vmem, vmem, hbm, hbm, hbm],
        out_specs=(vmem, vmem),
        scratch_shapes=[
            pltpu.VMEM((width, ff), BF16),
            pltpu.VMEM((width, ff), BF16),
            pltpu.VMEM((ff, width), BF16),
            pltpu.VMEM((n, rows, width), BF16),
            pltpu.VMEM((n * keys.shape[0], keys.shape[1]), BF16),
            pltpu.VMEM((n * values.shape[0], values.shape[1]), BF16),
            pltpu.VMEM((rows, ff), BF16),
            pltpu.VMEM((n, rows, width), BF16),
            pltpu.VMEM((n, 2, rows, cols), BF16),
            pltpu.VMEM((n, rows, cols), F32),
            pltpu.VMEM((n, rows, cols), BF16),
            pltpu.VMEM((n, rows, cols), BF16),
            pltpu.VMEM((n, rows, cols), BF16),
            pltpu.VMEM((n, rows, cols), BF16),
            dma((3,)),
            dma((2,)),
            dma((n,)),
            dma((n,)),
            dma((n,)),
            dma((n,)),
            dma((2, n)),
            dma((2, n)),
            dma((2, 2)),
            dma((2, n)),
            dma((2, n)),
            dma((2, n)),
            dma((2, n)),
            dma((n,)),
            dma((n,)),
            dma((n,)),
            dma((n,)),
        ],
        compiler_params=pltpu.CompilerParams(
            collective_id=0, has_side_effects=True, vmem_limit_bytes=60 * 1024 * 1024
        ),
        name="fused_layer",
    )(
        queries,
        keys,
        values,
        lambdas,
        head_gain.reshape(1, -1),
        tokens,
        route_ids,
        route_weights,
        moe_gain.reshape(1, -1),
        w_gate,
        w_up,
        w_down,
    )


def on_device(
    queries,
    keys,
    values,
    lambdas,
    head_gain,
    tokens,
    route_ids,
    route_weights,
    moe_gain,
    w_gate,
    w_up,
    w_down,
):
    rows = tokens.shape[0]
    expert_count = w_gate.shape[0] * lax.axis_size("ep")
    slots = 2 * rows * route_ids.shape[1] // expert_count
    if w_gate.shape[0] == 1 and lax.axis_size("tp") == 4 and slots >= rows:
        return fused(
            queries, keys, values, lambdas, head_gain, tokens,
            route_ids, route_weights, moe_gain, w_gate, w_up, w_down,
        )
    heads_out = attend(queries, keys, values, lambdas, head_gain)
    expert_out = experts(tokens, route_ids, route_weights, moe_gain, w_gate, w_up, w_down)
    return (heads_out, expert_out)


def solution(mesh):
    in_specs = (
        P(("grp", "ep"), "tp"),
        P(("grp", "ep"), "tp"),
        P(("grp", "ep"), "tp"),
        P("tp"),
        P(),
        P(("grp", "ep"), None),
        P(("grp", "ep"), None),
        P(("grp", "ep"), None),
        P(),
        P("ep", None, "tp"),
        P("ep", None, "tp"),
        P("ep", "tp", None),
    )
    out_specs = (P(("grp", "ep"), "tp"), P(("grp", "ep"), "tp"))
    return jax.shard_map(
        on_device, mesh=mesh, in_specs=in_specs, out_specs=out_specs, check_vma=False
    )
```

```python
import functools

import jax
import jax.numpy as jnp
from jax import lax
from jax.experimental import pallas as pl
from jax.experimental.pallas import tpu as pltpu
from jax.sharding import PartitionSpec as P

MESH = pl.DeviceIdType.MESH
F32 = jnp.float32
BF16 = jnp.bfloat16

def attend(queries, keys, values, lambdas, head_gain):
    row_count = queries.shape[0]
    head_count = lambdas.shape[0]
    head_dim = queries.shape[1] // (2 * head_count)
    value_dim = values.shape[1] // head_count
    query_parts = queries.reshape(row_count, head_count, 2, head_dim)
    score_scale = head_dim ** (-0.5)
    running = jnp.full((head_count, 2, row_count), -1e30, jnp.float32)
    key_piece = lax.all_gather(keys, "ep", axis=0, tiled=True)
    value_piece = lax.all_gather(values, "ep", axis=0, tiled=True)
    count = key_piece.shape[0]
    key_parts = key_piece.reshape(count, head_count, 2, head_dim)
    value_parts = value_piece.reshape(count, head_count, value_dim)
    scores = (
        jnp.einsum("qhcd,khcd->hcqk", query_parts, key_parts, preferred_element_type=jnp.float32)
        * score_scale
    )
    newest = jnp.maximum(running, jnp.max(scores, axis=-1))
    weights_now = jnp.exp(scores - newest[..., None])
    totals = jnp.sum(weights_now, axis=-1)
    sums = jnp.einsum(
        "hcqk,khe->hcqe",
        weights_now.astype(jnp.bfloat16),
        value_parts,
        preferred_element_type=jnp.float32,
    )
    running, totals, sums = (newest, totals, sums)
    means = sums / totals[..., None]
    mixed = means[:, 0] - lambdas[:, None, None] * means[:, 1]
    scaled = mixed * lax.rsqrt(jnp.mean(mixed * mixed, axis=-1, keepdims=True) + 1e-06) * head_gain
    return (
        jnp.transpose(scaled, (1, 0, 2))
        .reshape(row_count, head_count * value_dim)
        .astype(jnp.bfloat16)
    )


def experts(tokens, route_ids, route_weights, moe_gain, w_gate, w_up, w_down):
    row_count, width = tokens.shape
    top_count = route_ids.shape[1]
    ep_size = lax.axis_size("ep")
    tp_size = lax.axis_size("tp")
    expert_count = w_gate.shape[0] * ep_size
    capacity = 2 * row_count * top_count // expert_count
    token_float = tokens.astype(jnp.float32)
    normed = (
        token_float
        * lax.rsqrt(jnp.mean(token_float * token_float, axis=1, keepdims=True) + 1e-06)
        * moe_gain
    ).astype(jnp.bfloat16)
    flat_ids = route_ids.reshape(-1)
    onehot = (flat_ids[:, None] == jnp.arange(expert_count, dtype=jnp.int32)[None, :]).astype(
        jnp.int32
    )
    earlier = jnp.cumsum(onehot, axis=0) - onehot
    position = jnp.sum(earlier * onehot, axis=1)
    slot_index = flat_ids * capacity + position
    owners = (
        jnp.full((expert_count * capacity,), row_count, jnp.int32)
        .at[slot_index]
        .set(jnp.arange(row_count * top_count, dtype=jnp.int32) // top_count)
    )
    padded = jnp.concatenate([normed, jnp.zeros((1, width), jnp.bfloat16)], axis=0)
    outgoing = padded[owners].reshape(expert_count, capacity, width)
    gate_mat = w_gate[0]
    up_mat = w_up[0]
    down_mat = w_down[0]
    slice_width = width // tp_size
    own_columns = lax.dynamic_slice_in_dim(
        outgoing, lax.axis_index("tp") * slice_width, slice_width, 2
    )
    arrived = lax.all_to_all(own_columns, "ep", split_axis=0, concat_axis=0, tiled=True)
    piece = lax.all_gather(arrived, "tp", axis=2, tiled=True)
    gate = jnp.einsum("scd,df->scf", piece, gate_mat, preferred_element_type=jnp.float32)
    upward = jnp.einsum("scd,df->scf", piece, up_mat, preferred_element_type=jnp.float32)
    hidden = (jax.nn.silu(gate) * upward).astype(jnp.bfloat16)
    flat_hidden = hidden.reshape(-1, hidden.shape[2])
    summed = lax.psum_scatter(
        jnp.einsum("fd,sf->ds", down_mat, flat_hidden, preferred_element_type=jnp.float32).astype(
            jnp.bfloat16
        ),
        "tp",
        scatter_dimension=0,
        tiled=True,
    )
    back = lax.all_to_all(summed, "ep", split_axis=1, concat_axis=1, tiled=True)
    picked = (
        jnp.take(back, slot_index, axis=1).astype(jnp.float32).reshape(-1, row_count, top_count)
    )
    combined = jnp.einsum("drk,rk->rd", picked, route_weights)
    return combined.astype(jnp.bfloat16)


def visit_order(n):
    return [sorted((s for s in range(n) if s != e), key=lambda s: (abs(s - e), s)) for e in range(n)]


def fused_kernel(
    n,
    q_ref,
    k_ref,
    v_ref,
    lam_ref,
    hgain_ref,
    tok_ref,
    ids_ref,
    rw_ref,
    mgain_ref,
    wg_hbm,
    wu_hbm,
    wd_hbm,
    heads_ref,
    out_ref,
    wg,
    wu,
    wd,
    gathered,
    kbuf,
    vbuf,
    hid,
    part,
    core_in,
    s_own,
    s_out,
    x_in,
    t_out,
    ret,
    wsem,
    own_send,
    z_send,
    z_recv,
    x_send,
    x_recv,
    c_send,
    c_recv,
    kv_own,
    kv_send,
    kv_recv,
    r1_send,
    r1_recv,
    r2_send,
    r2_recv,
    r3_send,
    r3_recv,
):
    e = lax.axis_index("ep")
    t = lax.axis_index("tp")
    xi = t // 2
    ci = lax.rem(t, 2)
    core_peer = {"tp": 2 * xi + 1 - ci}
    x_peer = {"tp": 2 * (1 - xi) + ci}
    rows, width = tok_ref.shape
    cols = width // 4
    kv_rows = k_ref.shape[0]

    def colblock(j):
        return pl.ds(pl.multiple_of(j * cols, 128), cols)

    def remote(src, dst, ss, rs, dev):
        return pltpu.make_async_remote_copy(
            src_ref=src, dst_ref=dst, send_sem=ss, recv_sem=rs, device_id=dev, device_id_type=MESH
        )

    weights = [
        pltpu.make_async_copy(a, b, wsem.at[i])
        for i, (a, b) in enumerate(((wg_hbm.at[0], wg), (wu_hbm.at[0], wu), (wd_hbm.at[0], wd)))
    ]
    for c in weights:
        c.start()

    barrier = pltpu.get_barrier_semaphore()
    for d in range(1, n):
        pl.semaphore_signal(barrier, inc=1, device_id={"ep": lax.rem(e + d, n)}, device_id_type=MESH)
    pl.semaphore_signal(barrier, inc=1, device_id=core_peer, device_id_type=MESH)
    pl.semaphore_signal(barrier, inc=1, device_id=x_peer, device_id_type=MESH)

    halves = (0, 1)
    hr = rows // 2

    def half(h):
        return pl.ds(h * hr, hr)

    def normalize(h):
        step = 32

        @pl.loop(0, hr // step)
        def _(i):
            sl = pl.ds(pl.multiple_of(h * hr + i * step, step), step)
            v = tok_ref[sl, :].astype(F32)
            scale = lax.rsqrt(jnp.mean(v * v, axis=1, keepdims=True) + 1e-06)
            gathered[e, sl, :] = (v * scale * mgain_ref[...]).astype(BF16)

    has_left = e > 0
    has_right = e < n - 1
    sides = ((0, has_left, e - 1), (1, has_right, e + 1))
    own_kv = pl.ds(pl.multiple_of(e * kv_rows, kv_rows), kv_rows)

    def own_tok(side, peer, h):
        blk = gathered.at[e, half(h), colblock(t)]
        return remote(blk, blk, own_send.at[side, h], z_recv.at[e, h], {"ep": peer})

    def own_kv_copies(side, peer):
        dev = {"ep": peer}
        return (
            remote(k_ref, kbuf.at[own_kv], kv_own.at[0, side], kv_recv.at[0, e], dev),
            remote(v_ref, vbuf.at[own_kv], kv_own.at[1, side], kv_recv.at[1, e], dev),
        )

    orders = visit_order(n)

    def nth(k):
        s = jnp.int32(orders[0][k])
        for i in range(1, n):
            s = jnp.where(e == i, jnp.int32(orders[i][k]), s)
        return s

    visits = [nth(k) for k in range(n - 1)]

    def forward_of(s):
        from_left = s < e
        has = jnp.logical_or(
            jnp.logical_and(from_left, has_right),
            jnp.logical_and(jnp.logical_not(from_left), has_left),
        )
        return has, {"ep": jnp.clip(jnp.where(from_left, e + 1, e - 1), 0, n - 1)}

    def z_copy(s, h):
        blk = gathered.at[s, half(h), colblock(t)]
        return remote(blk, blk, z_send.at[s, h], z_recv.at[s, h], forward_of(s)[1])

    def x_copy(s, h):
        blk = gathered.at[s, half(h), colblock(t)]
        return remote(blk, blk, x_send.at[s, h], x_recv.at[s, h], x_peer)

    def c_copy(s, h, which):
        blk = gathered.at[s, half(h), colblock(t if which == 0 else 2 * (1 - xi) + ci)]
        return remote(blk, blk, c_send.at[which, s, h], c_recv.at[which, s, h], core_peer)

    def kv_copy(which, s):
        sl = pl.ds(pl.multiple_of(s * kv_rows, kv_rows), kv_rows)
        blk = (kbuf, vbuf)[which].at[sl]
        return remote(blk, blk, kv_send.at[which, s], kv_recv.at[which, s], forward_of(s)[1])

    def r1_copy(s, h, xx):
        return remote(
            part.at[s, half(h), colblock(2 * xx + 1 - ci)],
            core_in.at[s, xx, half(h)],
            r1_send.at[xx, s, h],
            r1_recv.at[xx, s, h],
            core_peer,
        )

    def r2_copy(s, h):
        return remote(
            s_out.at[s, half(h)], x_in.at[s, half(h)], r2_send.at[s, h], r2_recv.at[s, h], x_peer
        )

    def r3_copy(s, h):
        return remote(
            t_out.at[s, half(h)],
            ret.at[e, half(h)],
            r3_send.at[s, h],
            r3_recv.at[e, h],
            {"ep": s},
        )

    ff = wg.shape[1]
    nb = ff // 3
    ob = width // 3

    def up_step(s, b):
        sl = pl.ds(b * nb, nb)
        g = jnp.dot(gathered[s], wg[:, sl], preferred_element_type=F32)
        u = jnp.dot(gathered[s], wu[:, sl], preferred_element_type=F32)
        hid[:, sl] = (g / (1.0 + jnp.exp(-g)) * u).astype(BF16)

    def down_step(s, b):
        sl = pl.ds(b * ob, ob)
        part[s, :, sl] = jnp.dot(hid[...], wd[:, sl], preferred_element_type=F32).astype(BF16)

    def send_parts(s):
        for h in halves:
            r1_copy(s, h, 1 - xi).start()
        for h in halves:
            r1_copy(s, h, xi).start()

    def reduce_core(s):
        for h in halves:
            r1_copy(s, h, 1 - xi).wait_recv()
            s_out[s, half(h)] = (
                part[s, half(h), colblock(2 * (1 - xi) + ci)].astype(F32)
                + core_in[s, 1 - xi, half(h)].astype(F32)
            ).astype(BF16)
            r2_copy(s, h).start()
        for h in halves:
            r1_copy(s, h, xi).wait_recv()
        s_own[s] = part[s, :, colblock(t)].astype(F32) + core_in[s, xi].astype(F32)

    def reduce_x(s, send=True):
        for h in halves:
            r2_copy(s, h).wait_recv()
            t_out[s, half(h)] = (s_own[s, half(h)] + x_in[s, half(h)].astype(F32)).astype(BF16)
            if send:
                r3_copy(s, h).start()

    def arrive(s, h):
        z_copy(s, h).wait_recv()

        @pl.when(forward_of(s)[0])
        def _():
            z_copy(s, h).start()

        x_copy(s, h).start()
        c_copy(s, h, 0).start()

    def cross(s, h):
        x_copy(s, h).wait_recv()
        c_copy(s, h, 1).start()

    def ready(s):
        for h in halves:
            c_copy(s, h, 0).wait_recv()
            c_copy(s, h, 1).wait_recv()

    def relay_kv(s):
        for w in (0, 1):
            kv_copy(w, s).wait_recv()

            @pl.when(forward_of(s)[0])
            def _():
                kv_copy(w, s).start()

    def attend(h):
        heads = lam_ref.shape[0]
        vd = v_ref.shape[1] // heads
        hd = q_ref.shape[1] // (2 * heads)
        qr = q_ref.shape[0]
        first = lax.broadcasted_iota(jnp.int32, (qr, 2 * hd), 1) < hd
        q = q_ref[:, h * 2 * hd : (h + 1) * 2 * hd].astype(F32)
        both = jnp.concatenate(
            [jnp.where(first, q, 0.0).astype(BF16), jnp.where(first, 0.0, q).astype(BF16)], axis=0
        )
        kh = kbuf[:, h * 2 * hd : (h + 1) * 2 * hd]
        vh = vbuf[:, h * vd : (h + 1) * vd]
        scores = lax.dot_general(
            both, kh, (((1,), (1,)), ((), ())), preferred_element_type=F32
        ) * (hd ** (-0.5))
        ex = jnp.exp(scores - jnp.max(scores, axis=1, keepdims=True))
        tot = jnp.sum(ex, axis=1, keepdims=True)
        sums = jnp.dot(ex.astype(BF16), vh, preferred_element_type=F32) / tot
        mixed = sums[:qr] - lam_ref[h] * sums[qr:]
        norm = lax.rsqrt(jnp.mean(mixed * mixed, axis=1, keepdims=True) + 1e-06)
        heads_ref[:, h * vd : (h + 1) * vd] = (mixed * norm * hgain_ref[...]).astype(BF16)

    for h in halves:
        normalize(h)
        if h == 0:
            pl.semaphore_wait(barrier, n + 1)
        for side, has, peer in sides:

            @pl.when(has)
            def _():
                own_tok(side, peer, h).start()

    kbuf[own_kv, :] = k_ref[...]
    vbuf[own_kv, :] = v_ref[...]

    def send_kv():
        for side, has, peer in sides:

            @pl.when(has)
            def _():
                for c in own_kv_copies(side, peer):
                    c.start()

    last = len(visits) - 1
    for c in weights:
        c.wait()
    for b in range(3):
        up_step(e, b)
    for b in range(3):
        down_step(e, b)
    send_parts(e)
    for h in halves:
        arrive(visits[0], h)
    for h in halves:
        cross(visits[0], h)
        if last >= 1:
            arrive(visits[1], h)
    ready(visits[0])
    for k, s in enumerate(visits):
        ahead = visits[k + 1] if k < last else None
        further = visits[k + 2] if k + 1 < last else None
        before = visits[k - 1] if k > 0 else None
        up_step(s, 0)
        if ahead is not None:
            cross(ahead, 0)
        if further is not None:
            arrive(further, 0)
        up_step(s, 1)
        if ahead is not None:
            cross(ahead, 1)
        if further is not None:
            arrive(further, 1)
        if k == max(last - 2, 0):
            send_kv()
        up_step(s, 2)
        if before is not None:
            reduce_core(before)
            relay_kv(before)
        for b in range(3):
            down_step(s, b)
        send_parts(s)
        if ahead is not None:
            ready(ahead)
    for k in range(max(last - 1, 0)):
        reduce_x(visits[k])
    reduce_core(visits[last])
    reduce_core(e)
    relay_kv(visits[last])
    heads = lam_ref.shape[0]
    attend(0)
    if last >= 1:
        reduce_x(visits[last - 1])
    for h in range(1, heads):
        attend(h)
    reduce_x(visits[last])
    reduce_x(e, send=False)

    ids = ids_ref[...]
    rw = rw_ref[...]

    def weight_of(x):
        return jnp.sum(jnp.where(ids == x, rw, 0.0), axis=1, keepdims=True)

    total = t_out[e].astype(F32) * weight_of(e)
    for s in visits:
        for h in halves:
            remote(
                t_out.at[s, half(h)],
                ret.at[s, half(h)],
                r3_send.at[s, h],
                r3_recv.at[s, h],
                {"ep": s},
            ).wait_recv()
        total = total + ret[s].astype(F32) * weight_of(s)
    out_ref[...] = total.astype(BF16)

    for side, has, peer in sides:

        @pl.when(has)
        def _():
            for h in halves:
                own_tok(side, peer, h).wait_send()
            for c in own_kv_copies(side, peer):
                c.wait_send()

    for s in [e] + visits:
        for h in halves:
            r1_copy(s, h, 1 - xi).wait_send()
            r1_copy(s, h, xi).wait_send()
            r2_copy(s, h).wait_send()
    for s in visits:
        for h in halves:
            x_copy(s, h).wait_send()
            c_copy(s, h, 0).wait_send()
            c_copy(s, h, 1).wait_send()
            r3_copy(s, h).wait_send()

        @pl.when(forward_of(s)[0])
        def _():
            for h in halves:
                z_copy(s, h).wait_send()
            kv_copy(0, s).wait_send()
            kv_copy(1, s).wait_send()


def fused(queries, keys, values, lambdas, head_gain, tokens, route_ids, route_weights, moe_gain, w_gate, w_up, w_down):
    n = lax.axis_size("ep")
    rows, width = tokens.shape
    cols = width // 4
    ff = w_gate.shape[2]
    vmem = pl.BlockSpec(memory_space=pltpu.VMEM)
    smem = pl.BlockSpec(memory_space=pltpu.SMEM)
    hbm = pl.BlockSpec(memory_space=pl.ANY)
    dma = pltpu.SemaphoreType.DMA
    return pl.pallas_call(
        functools.partial(fused_kernel, n),
        out_shape=(
            jax.ShapeDtypeStruct((queries.shape[0], values.shape[1]), BF16),
            jax.ShapeDtypeStruct((rows, cols), BF16),
        ),
        in_specs=[vmem, vmem, vmem, smem, vmem, vmem, vmem, vmem, vmem, hbm, hbm, hbm],
        out_specs=(vmem, vmem),
        scratch_shapes=[
            pltpu.VMEM((width, ff), BF16),
            pltpu.VMEM((width, ff), BF16),
            pltpu.VMEM((ff, width), BF16),
            pltpu.VMEM((n, rows, width), BF16),
            pltpu.VMEM((n * keys.shape[0], keys.shape[1]), BF16),
            pltpu.VMEM((n * values.shape[0], values.shape[1]), BF16),
            pltpu.VMEM((rows, ff), BF16),
            pltpu.VMEM((n, rows, width), BF16),
            pltpu.VMEM((n, 2, rows, cols), BF16),
            pltpu.VMEM((n, rows, cols), F32),
            pltpu.VMEM((n, rows, cols), BF16),
            pltpu.VMEM((n, rows, cols), BF16),
            pltpu.VMEM((n, rows, cols), BF16),
            pltpu.VMEM((n, rows, cols), BF16),
            dma((3,)),
            dma((2, 2)),
            dma((n, 2)),
            dma((n, 2)),
            dma((n, 2)),
            dma((n, 2)),
            dma((2, n, 2)),
            dma((2, n, 2)),
            dma((2, 2)),
            dma((2, n)),
            dma((2, n)),
            dma((2, n, 2)),
            dma((2, n, 2)),
            dma((n, 2)),
            dma((n, 2)),
            dma((n, 2)),
            dma((n, 2)),
        ],
        compiler_params=pltpu.CompilerParams(
            collective_id=0, has_side_effects=True, vmem_limit_bytes=60 * 1024 * 1024
        ),
        name="fused_layer",
    )(
        queries,
        keys,
        values,
        lambdas,
        head_gain.reshape(1, -1),
        tokens,
        route_ids,
        route_weights,
        moe_gain.reshape(1, -1),
        w_gate,
        w_up,
        w_down,
    )


def on_device(
    queries,
    keys,
    values,
    lambdas,
    head_gain,
    tokens,
    route_ids,
    route_weights,
    moe_gain,
    w_gate,
    w_up,
    w_down,
):
    rows = tokens.shape[0]
    expert_count = w_gate.shape[0] * lax.axis_size("ep")
    slots = 2 * rows * route_ids.shape[1] // expert_count
    if w_gate.shape[0] == 1 and lax.axis_size("tp") == 4 and slots >= rows:
        return fused(
            queries, keys, values, lambdas, head_gain, tokens,
            route_ids, route_weights, moe_gain, w_gate, w_up, w_down,
        )
    heads_out = attend(queries, keys, values, lambdas, head_gain)
    expert_out = experts(tokens, route_ids, route_weights, moe_gain, w_gate, w_up, w_down)
    return (heads_out, expert_out)


def solution(mesh):
    in_specs = (
        P(("grp", "ep"), "tp"),
        P(("grp", "ep"), "tp"),
        P(("grp", "ep"), "tp"),
        P("tp"),
        P(),
        P(("grp", "ep"), None),
        P(("grp", "ep"), None),
        P(("grp", "ep"), None),
        P(),
        P("ep", None, "tp"),
        P("ep", None, "tp"),
        P("ep", "tp", None),
    )
    out_specs = (P(("grp", "ep"), "tp"), P(("grp", "ep"), "tp"))
    return jax.shard_map(
        on_device, mesh=mesh, in_specs=in_specs, out_specs=out_specs, check_vma=False
    )
```

```python
import functools

import jax
import jax.numpy as jnp
from jax import lax
from jax.experimental import pallas as pl
from jax.experimental.pallas import tpu as pltpu
from jax.sharding import PartitionSpec as P

MESH = pl.DeviceIdType.MESH
F32 = jnp.float32
BF16 = jnp.bfloat16

def attend(queries, keys, values, lambdas, head_gain):
    row_count = queries.shape[0]
    head_count = lambdas.shape[0]
    head_dim = queries.shape[1] // (2 * head_count)
    value_dim = values.shape[1] // head_count
    query_parts = queries.reshape(row_count, head_count, 2, head_dim)
    score_scale = head_dim ** (-0.5)
    running = jnp.full((head_count, 2, row_count), -1e30, jnp.float32)
    key_piece = lax.all_gather(keys, "ep", axis=0, tiled=True)
    value_piece = lax.all_gather(values, "ep", axis=0, tiled=True)
    count = key_piece.shape[0]
    key_parts = key_piece.reshape(count, head_count, 2, head_dim)
    value_parts = value_piece.reshape(count, head_count, value_dim)
    scores = (
        jnp.einsum("qhcd,khcd->hcqk", query_parts, key_parts, preferred_element_type=jnp.float32)
        * score_scale
    )
    newest = jnp.maximum(running, jnp.max(scores, axis=-1))
    weights_now = jnp.exp(scores - newest[..., None])
    totals = jnp.sum(weights_now, axis=-1)
    sums = jnp.einsum(
        "hcqk,khe->hcqe",
        weights_now.astype(jnp.bfloat16),
        value_parts,
        preferred_element_type=jnp.float32,
    )
    running, totals, sums = (newest, totals, sums)
    means = sums / totals[..., None]
    mixed = means[:, 0] - lambdas[:, None, None] * means[:, 1]
    scaled = mixed * lax.rsqrt(jnp.mean(mixed * mixed, axis=-1, keepdims=True) + 1e-06) * head_gain
    return (
        jnp.transpose(scaled, (1, 0, 2))
        .reshape(row_count, head_count * value_dim)
        .astype(jnp.bfloat16)
    )


def experts(tokens, route_ids, route_weights, moe_gain, w_gate, w_up, w_down):
    row_count, width = tokens.shape
    top_count = route_ids.shape[1]
    ep_size = lax.axis_size("ep")
    tp_size = lax.axis_size("tp")
    expert_count = w_gate.shape[0] * ep_size
    capacity = 2 * row_count * top_count // expert_count
    token_float = tokens.astype(jnp.float32)
    normed = (
        token_float
        * lax.rsqrt(jnp.mean(token_float * token_float, axis=1, keepdims=True) + 1e-06)
        * moe_gain
    ).astype(jnp.bfloat16)
    flat_ids = route_ids.reshape(-1)
    onehot = (flat_ids[:, None] == jnp.arange(expert_count, dtype=jnp.int32)[None, :]).astype(
        jnp.int32
    )
    earlier = jnp.cumsum(onehot, axis=0) - onehot
    position = jnp.sum(earlier * onehot, axis=1)
    slot_index = flat_ids * capacity + position
    owners = (
        jnp.full((expert_count * capacity,), row_count, jnp.int32)
        .at[slot_index]
        .set(jnp.arange(row_count * top_count, dtype=jnp.int32) // top_count)
    )
    padded = jnp.concatenate([normed, jnp.zeros((1, width), jnp.bfloat16)], axis=0)
    outgoing = padded[owners].reshape(expert_count, capacity, width)
    gate_mat = w_gate[0]
    up_mat = w_up[0]
    down_mat = w_down[0]
    slice_width = width // tp_size
    own_columns = lax.dynamic_slice_in_dim(
        outgoing, lax.axis_index("tp") * slice_width, slice_width, 2
    )
    arrived = lax.all_to_all(own_columns, "ep", split_axis=0, concat_axis=0, tiled=True)
    piece = lax.all_gather(arrived, "tp", axis=2, tiled=True)
    gate = jnp.einsum("scd,df->scf", piece, gate_mat, preferred_element_type=jnp.float32)
    upward = jnp.einsum("scd,df->scf", piece, up_mat, preferred_element_type=jnp.float32)
    hidden = (jax.nn.silu(gate) * upward).astype(jnp.bfloat16)
    flat_hidden = hidden.reshape(-1, hidden.shape[2])
    summed = lax.psum_scatter(
        jnp.einsum("fd,sf->ds", down_mat, flat_hidden, preferred_element_type=jnp.float32).astype(
            jnp.bfloat16
        ),
        "tp",
        scatter_dimension=0,
        tiled=True,
    )
    back = lax.all_to_all(summed, "ep", split_axis=1, concat_axis=1, tiled=True)
    picked = (
        jnp.take(back, slot_index, axis=1).astype(jnp.float32).reshape(-1, row_count, top_count)
    )
    combined = jnp.einsum("drk,rk->rd", picked, route_weights)
    return combined.astype(jnp.bfloat16)


def visit_order(n):
    return [sorted((s for s in range(n) if s != e), key=lambda s: (abs(s - e), s)) for e in range(n)]


def fused_kernel(
    n,
    q_ref,
    k_ref,
    v_ref,
    lam_ref,
    hgain_ref,
    tok_ref,
    ids_ref,
    rw_ref,
    mgain_ref,
    wg_hbm,
    wu_hbm,
    wd_hbm,
    heads_ref,
    out_ref,
    wg,
    wu,
    wd,
    gathered,
    kbuf,
    vbuf,
    hid,
    part,
    core_in,
    s_own,
    s_out,
    x_in,
    t_out,
    ret,
    out_weights,
    wsem,
    own_send,
    z_send,
    z_recv,
    x_send,
    x_recv,
    c_send,
    c_recv,
    kv_send,
    kv_recv,
    r1_send,
    r1_recv,
    r2_send,
    r2_recv,
    r3_send,
    r3_recv,
):
    e = lax.axis_index("ep")
    t = lax.axis_index("tp")
    xi = t // 2
    ci = lax.rem(t, 2)
    core_peer = {"tp": 2 * xi + 1 - ci}
    x_peer = {"tp": 2 * (1 - xi) + ci}
    rows, width = tok_ref.shape
    cols = width // 4
    kv_rows = k_ref.shape[0]

    def colblock(j):
        return pl.ds(pl.multiple_of(j * cols, 128), cols)

    def remote(src, dst, ss, rs, dev):
        return pltpu.make_async_remote_copy(
            src_ref=src, dst_ref=dst, send_sem=ss, recv_sem=rs, device_id=dev, device_id_type=MESH
        )

    weights = [
        pltpu.make_async_copy(a, b, wsem.at[i])
        for i, (a, b) in enumerate(((wg_hbm.at[0], wg), (wu_hbm.at[0], wu), (wd_hbm.at[0], wd)))
    ]
    for c in weights:
        c.start()

    barrier = pltpu.get_barrier_semaphore()
    for d in range(1, n):
        pl.semaphore_signal(barrier, inc=1, device_id={"ep": lax.rem(e + d, n)}, device_id_type=MESH)
    pl.semaphore_signal(barrier, inc=1, device_id=core_peer, device_id_type=MESH)
    pl.semaphore_signal(barrier, inc=1, device_id=x_peer, device_id_type=MESH)

    halves = (0, 1)
    hr = rows // 2

    def half(h):
        return pl.ds(h * hr, hr)

    def normalize(h):
        step = 32

        @pl.loop(0, hr // step)
        def _(i):
            sl = pl.ds(pl.multiple_of(h * hr + i * step, step), step)
            v = tok_ref[sl, :].astype(F32)
            scale = lax.rsqrt(jnp.mean(v * v, axis=1, keepdims=True) + 1e-06)
            gathered[e, sl, :] = (v * scale * mgain_ref[...]).astype(BF16)

    has_left = e > 0
    has_right = e < n - 1
    sides = ((0, has_left, e - 1), (1, has_right, e + 1))
    own_kv = pl.ds(pl.multiple_of(e * kv_rows, kv_rows), kv_rows)

    def own_tok(side, peer, h):
        blk = gathered.at[e, half(h), colblock(t)]
        return remote(blk, blk, own_send.at[side, h], z_recv.at[e, h], {"ep": peer})

    def kv_copies(s):
        dev = {"ep": s}
        return (
            remote(k_ref, kbuf.at[own_kv], kv_send.at[0, s], kv_recv.at[0, e], dev),
            remote(v_ref, vbuf.at[own_kv], kv_send.at[1, s], kv_recv.at[1, e], dev),
        )

    def kv_arrivals(s):
        sl = pl.ds(pl.multiple_of(s * kv_rows, kv_rows), kv_rows)
        return (
            remote(k_ref, kbuf.at[sl], kv_send.at[0, s], kv_recv.at[0, s], {"ep": s}),
            remote(v_ref, vbuf.at[sl], kv_send.at[1, s], kv_recv.at[1, s], {"ep": s}),
        )

    orders = visit_order(n)

    def nth(k):
        s = jnp.int32(orders[0][k])
        for i in range(1, n):
            s = jnp.where(e == i, jnp.int32(orders[i][k]), s)
        return s

    visits = [nth(k) for k in range(n - 1)]

    def forward_of(s):
        from_left = s < e
        has = jnp.logical_or(
            jnp.logical_and(from_left, has_right),
            jnp.logical_and(jnp.logical_not(from_left), has_left),
        )
        return has, {"ep": jnp.clip(jnp.where(from_left, e + 1, e - 1), 0, n - 1)}

    def z_copy(s, h):
        blk = gathered.at[s, half(h), colblock(t)]
        return remote(blk, blk, z_send.at[s, h], z_recv.at[s, h], forward_of(s)[1])

    def x_copy(s, h):
        blk = gathered.at[s, half(h), colblock(t)]
        return remote(blk, blk, x_send.at[s, h], x_recv.at[s, h], x_peer)

    def c_copy(s, h, which):
        blk = gathered.at[s, half(h), colblock(t if which == 0 else 2 * (1 - xi) + ci)]
        return remote(blk, blk, c_send.at[which, s, h], c_recv.at[which, s, h], core_peer)

    def r1_copy(s, h, xx):
        return remote(
            part.at[s, half(h), colblock(2 * xx + 1 - ci)],
            core_in.at[s, xx, half(h)],
            r1_send.at[xx, s, h],
            r1_recv.at[xx, s, h],
            core_peer,
        )

    def r2_copy(s, h):
        return remote(
            s_out.at[s, half(h)], x_in.at[s, half(h)], r2_send.at[s, h], r2_recv.at[s, h], x_peer
        )

    def r3_copy(s, h):
        return remote(
            t_out.at[s, half(h)],
            ret.at[e, half(h)],
            r3_send.at[s, h],
            r3_recv.at[e, h],
            {"ep": s},
        )

    ff = wg.shape[1]
    nb = ff // 3
    ob = width // 3

    def up_step(s, b):
        sl = pl.ds(b * nb, nb)
        g = jnp.dot(gathered[s], wg[:, sl], preferred_element_type=F32)
        u = jnp.dot(gathered[s], wu[:, sl], preferred_element_type=F32)
        hid[:, sl] = (g / (1.0 + jnp.exp(-g)) * u).astype(BF16)

    def down_step(s, b):
        sl = pl.ds(b * ob, ob)
        part[s, :, sl] = jnp.dot(hid[...], wd[:, sl], preferred_element_type=F32).astype(BF16)

    def send_parts(s):
        for h in halves:
            r1_copy(s, h, 1 - xi).start()
        for h in halves:
            r1_copy(s, h, xi).start()

    def reduce_core(s):
        for h in halves:
            r1_copy(s, h, 1 - xi).wait_recv()
            s_out[s, half(h)] = (
                part[s, half(h), colblock(2 * (1 - xi) + ci)].astype(F32)
                + core_in[s, 1 - xi, half(h)].astype(F32)
            ).astype(BF16)
            r2_copy(s, h).start()
        for h in halves:
            r1_copy(s, h, xi).wait_recv()
        s_own[s] = part[s, :, colblock(t)].astype(F32) + core_in[s, xi].astype(F32)

    def reduce_x(s, send=True):
        for h in halves:
            r2_copy(s, h).wait_recv()
            t_out[s, half(h)] = (s_own[s, half(h)] + x_in[s, half(h)].astype(F32)).astype(BF16)
            if send:
                r3_copy(s, h).start()

    def arrive(s, h):
        z_copy(s, h).wait_recv()

        @pl.when(forward_of(s)[0])
        def _():
            z_copy(s, h).start()

        x_copy(s, h).start()
        c_copy(s, h, 0).start()

    def cross(s, h):
        x_copy(s, h).wait_recv()
        c_copy(s, h, 1).start()

    def ready(s):
        for h in halves:
            c_copy(s, h, 0).wait_recv()
            c_copy(s, h, 1).wait_recv()

    def attend(h):
        heads = lam_ref.shape[0]
        vd = v_ref.shape[1] // heads
        hd = q_ref.shape[1] // (2 * heads)
        qr = q_ref.shape[0]
        first = lax.broadcasted_iota(jnp.int32, (qr, 2 * hd), 1) < hd
        q = q_ref[:, h * 2 * hd : (h + 1) * 2 * hd].astype(F32)
        both = jnp.concatenate(
            [jnp.where(first, q, 0.0).astype(BF16), jnp.where(first, 0.0, q).astype(BF16)], axis=0
        )
        kh = kbuf[:, h * 2 * hd : (h + 1) * 2 * hd]
        vh = vbuf[:, h * vd : (h + 1) * vd]
        scores = lax.dot_general(
            both, kh, (((1,), (1,)), ((), ())), preferred_element_type=F32
        ) * (hd ** (-0.5))
        ex = jnp.exp(scores - jnp.max(scores, axis=1, keepdims=True))
        tot = jnp.sum(ex, axis=1, keepdims=True)
        sums = jnp.dot(ex.astype(BF16), vh, preferred_element_type=F32) / tot
        mixed = sums[:qr] - lam_ref[h] * sums[qr:]
        norm = lax.rsqrt(jnp.mean(mixed * mixed, axis=1, keepdims=True) + 1e-06)
        heads_ref[:, h * vd : (h + 1) * vd] = (mixed * norm * hgain_ref[...]).astype(BF16)

    for h in halves:
        normalize(h)
        if h == 0:
            pl.semaphore_wait(barrier, n + 1)
        for side, has, peer in sides:

            @pl.when(has)
            def _():
                own_tok(side, peer, h).start()

    kbuf[own_kv, :] = k_ref[...]
    vbuf[own_kv, :] = v_ref[...]

    def send_kv():
        for s in visits:
            for c in kv_copies(s):
                c.start()

    ids = ids_ref[...]
    rw = rw_ref[...]
    lines = [jnp.sum(jnp.where(ids == x, rw, 0.0), axis=0, keepdims=True) for x in [e] + visits]
    pad = (-len(lines)) % 8
    lines.append(jnp.zeros((pad, rows), F32))
    out_weights[...] = jnp.concatenate(lines, axis=0).T

    last = len(visits) - 1
    for c in weights:
        c.wait()
    for b in range(3):
        up_step(e, b)
    for b in range(3):
        down_step(e, b)
    send_parts(e)
    for h in halves:
        arrive(visits[0], h)
    for h in halves:
        cross(visits[0], h)
        if last >= 1:
            arrive(visits[1], h)
    ready(visits[0])
    for k, s in enumerate(visits):
        ahead = visits[k + 1] if k < last else None
        further = visits[k + 2] if k + 1 < last else None
        before = visits[k - 1] if k > 0 else None
        up_step(s, 0)
        if ahead is not None:
            cross(ahead, 0)
        if further is not None:
            arrive(further, 0)
        up_step(s, 1)
        if ahead is not None:
            cross(ahead, 1)
        if further is not None:
            arrive(further, 1)
        if k == max(last - 2, 0):
            send_kv()
        up_step(s, 2)
        if before is not None:
            reduce_core(before)
        for b in range(3):
            down_step(s, b)
        send_parts(s)
        if ahead is not None:
            ready(ahead)
    for k in range(max(last - 1, 0)):
        reduce_x(visits[k])
    reduce_core(visits[last])
    reduce_core(e)
    heads = lam_ref.shape[0]
    for s in visits:
        for c in kv_arrivals(s):
            c.wait_recv()
    attend(0)
    if last >= 1:
        reduce_x(visits[last - 1])
    for h in range(1, heads):
        attend(h)
    reduce_x(visits[last])
    reduce_x(e, send=False)

    total = out_weights[:, 0:1] * t_out[e].astype(F32)
    for k, s in enumerate(visits):
        for h in halves:
            remote(
                t_out.at[s, half(h)],
                ret.at[s, half(h)],
                r3_send.at[s, h],
                r3_recv.at[s, h],
                {"ep": s},
            ).wait_recv()
        total = total + ret[s].astype(F32) * out_weights[:, k + 1 : k + 2]
    out_ref[...] = total.astype(BF16)

    for side, has, peer in sides:

        @pl.when(has)
        def _():
            for h in halves:
                own_tok(side, peer, h).wait_send()

    for s in [e] + visits:
        for h in halves:
            r1_copy(s, h, 1 - xi).wait_send()
            r1_copy(s, h, xi).wait_send()
            r2_copy(s, h).wait_send()
    for s in visits:
        for h in halves:
            x_copy(s, h).wait_send()
            c_copy(s, h, 0).wait_send()
            c_copy(s, h, 1).wait_send()
            r3_copy(s, h).wait_send()
        for c in kv_copies(s):
            c.wait_send()

        @pl.when(forward_of(s)[0])
        def _():
            for h in halves:
                z_copy(s, h).wait_send()


def hand_on_kernel(a_ref, b_ref, c_ref, d_ref):
    c_ref[...] = a_ref[...]
    d_ref[...] = b_ref[...]


def fused(queries, keys, values, lambdas, head_gain, tokens, route_ids, route_weights, moe_gain, w_gate, w_up, w_down):
    n = lax.axis_size("ep")
    rows, width = tokens.shape
    cols = width // 4
    ff = w_gate.shape[2]
    vmem = pl.BlockSpec(memory_space=pltpu.VMEM)
    smem = pl.BlockSpec(memory_space=pltpu.SMEM)
    hbm = pl.BlockSpec(memory_space=pl.ANY)
    dma = pltpu.SemaphoreType.DMA
    results = pl.pallas_call(
        functools.partial(fused_kernel, n),
        out_shape=(
            jax.ShapeDtypeStruct((queries.shape[0], values.shape[1]), BF16),
            jax.ShapeDtypeStruct((rows, cols), BF16),
        ),
        in_specs=[vmem, vmem, vmem, smem, vmem, vmem, vmem, vmem, vmem, hbm, hbm, hbm],
        out_specs=(vmem, vmem),
        scratch_shapes=[
            pltpu.VMEM((width, ff), BF16),
            pltpu.VMEM((width, ff), BF16),
            pltpu.VMEM((ff, width), BF16),
            pltpu.VMEM((n, rows, width), BF16),
            pltpu.VMEM((n * keys.shape[0], keys.shape[1]), BF16),
            pltpu.VMEM((n * values.shape[0], values.shape[1]), BF16),
            pltpu.VMEM((rows, ff), BF16),
            pltpu.VMEM((n, rows, width), BF16),
            pltpu.VMEM((n, 2, rows, cols), BF16),
            pltpu.VMEM((n, rows, cols), F32),
            pltpu.VMEM((n, rows, cols), BF16),
            pltpu.VMEM((n, rows, cols), BF16),
            pltpu.VMEM((n, rows, cols), BF16),
            pltpu.VMEM((n, rows, cols), BF16),
            pltpu.VMEM((rows, -(-n // 8) * 8), F32),
            dma((3,)),
            dma((2, 2)),
            dma((n, 2)),
            dma((n, 2)),
            dma((n, 2)),
            dma((n, 2)),
            dma((2, n, 2)),
            dma((2, n, 2)),
            dma((2, n)),
            dma((2, n)),
            dma((2, n, 2)),
            dma((2, n, 2)),
            dma((n, 2)),
            dma((n, 2)),
            dma((n, 2)),
            dma((n, 2)),
        ],
        compiler_params=pltpu.CompilerParams(
            collective_id=0, has_side_effects=True, vmem_limit_bytes=60 * 1024 * 1024
        ),
        name="fused_layer",
    )(
        queries,
        keys,
        values,
        lambdas,
        head_gain,
        tokens,
        route_ids.T,
        route_weights.T,
        moe_gain,
        w_gate,
        w_up,
        w_down,
    )
    return pl.pallas_call(
        hand_on_kernel,
        out_shape=tuple(jax.ShapeDtypeStruct(r.shape, r.dtype) for r in results),
        in_specs=[vmem, vmem],
        out_specs=(vmem, vmem),
        name="hand_on",
    )(*results)


def on_device(
    queries,
    keys,
    values,
    lambdas,
    head_gain,
    tokens,
    route_ids,
    route_weights,
    moe_gain,
    w_gate,
    w_up,
    w_down,
):
    rows = tokens.shape[0]
    expert_count = w_gate.shape[0] * lax.axis_size("ep")
    slots = 2 * rows * route_ids.shape[1] // expert_count
    if w_gate.shape[0] == 1 and lax.axis_size("tp") == 4 and slots >= rows:
        return fused(
            queries, keys, values, lambdas, head_gain, tokens,
            route_ids, route_weights, moe_gain, w_gate, w_up, w_down,
        )
    heads_out = attend(queries, keys, values, lambdas, head_gain)
    expert_out = experts(tokens, route_ids, route_weights, moe_gain, w_gate, w_up, w_down)
    return (heads_out, expert_out)


def solution(mesh):
    in_specs = (
        P(("grp", "ep"), "tp"),
        P(("grp", "ep"), "tp"),
        P(("grp", "ep"), "tp"),
        P("tp"),
        P(),
        P(("grp", "ep"), None),
        P(("grp", "ep"), None),
        P(("grp", "ep"), None),
        P(),
        P("ep", None, "tp"),
        P("ep", None, "tp"),
        P("ep", "tp", None),
    )
    out_specs = (P(("grp", "ep"), "tp"), P(("grp", "ep"), "tp"))
    return jax.shard_map(
        on_device, mesh=mesh, in_specs=in_specs, out_specs=out_specs, check_vma=False
    )
```

```python
import functools

import jax
import jax.numpy as jnp
from jax import lax
from jax.experimental import pallas as pl
from jax.experimental.pallas import tpu as pltpu
from jax.sharding import PartitionSpec as P

MESH = pl.DeviceIdType.MESH
F32 = jnp.float32
BF16 = jnp.bfloat16
PIECES = 2

def attend(queries, keys, values, lambdas, head_gain):
    row_count = queries.shape[0]
    head_count = lambdas.shape[0]
    head_dim = queries.shape[1] // (2 * head_count)
    value_dim = values.shape[1] // head_count
    query_parts = queries.reshape(row_count, head_count, 2, head_dim)
    score_scale = head_dim ** (-0.5)
    running = jnp.full((head_count, 2, row_count), -1e30, jnp.float32)
    key_piece = lax.all_gather(keys, "ep", axis=0, tiled=True)
    value_piece = lax.all_gather(values, "ep", axis=0, tiled=True)
    count = key_piece.shape[0]
    key_parts = key_piece.reshape(count, head_count, 2, head_dim)
    value_parts = value_piece.reshape(count, head_count, value_dim)
    scores = (
        jnp.einsum("qhcd,khcd->hcqk", query_parts, key_parts, preferred_element_type=jnp.float32)
        * score_scale
    )
    newest = jnp.maximum(running, jnp.max(scores, axis=-1))
    weights_now = jnp.exp(scores - newest[..., None])
    totals = jnp.sum(weights_now, axis=-1)
    sums = jnp.einsum(
        "hcqk,khe->hcqe",
        weights_now.astype(jnp.bfloat16),
        value_parts,
        preferred_element_type=jnp.float32,
    )
    running, totals, sums = (newest, totals, sums)
    means = sums / totals[..., None]
    mixed = means[:, 0] - lambdas[:, None, None] * means[:, 1]
    scaled = mixed * lax.rsqrt(jnp.mean(mixed * mixed, axis=-1, keepdims=True) + 1e-06) * head_gain
    return (
        jnp.transpose(scaled, (1, 0, 2))
        .reshape(row_count, head_count * value_dim)
        .astype(jnp.bfloat16)
    )


def experts(tokens, route_ids, route_weights, moe_gain, w_gate, w_up, w_down):
    row_count, width = tokens.shape
    top_count = route_ids.shape[1]
    ep_size = lax.axis_size("ep")
    tp_size = lax.axis_size("tp")
    expert_count = w_gate.shape[0] * ep_size
    capacity = 2 * row_count * top_count // expert_count
    token_float = tokens.astype(jnp.float32)
    normed = (
        token_float
        * lax.rsqrt(jnp.mean(token_float * token_float, axis=1, keepdims=True) + 1e-06)
        * moe_gain
    ).astype(jnp.bfloat16)
    flat_ids = route_ids.reshape(-1)
    onehot = (flat_ids[:, None] == jnp.arange(expert_count, dtype=jnp.int32)[None, :]).astype(
        jnp.int32
    )
    earlier = jnp.cumsum(onehot, axis=0) - onehot
    position = jnp.sum(earlier * onehot, axis=1)
    slot_index = flat_ids * capacity + position
    owners = (
        jnp.full((expert_count * capacity,), row_count, jnp.int32)
        .at[slot_index]
        .set(jnp.arange(row_count * top_count, dtype=jnp.int32) // top_count)
    )
    padded = jnp.concatenate([normed, jnp.zeros((1, width), jnp.bfloat16)], axis=0)
    outgoing = padded[owners].reshape(expert_count, capacity, width)
    gate_mat = w_gate[0]
    up_mat = w_up[0]
    down_mat = w_down[0]
    slice_width = width // tp_size
    own_columns = lax.dynamic_slice_in_dim(
        outgoing, lax.axis_index("tp") * slice_width, slice_width, 2
    )
    arrived = lax.all_to_all(own_columns, "ep", split_axis=0, concat_axis=0, tiled=True)
    piece = lax.all_gather(arrived, "tp", axis=2, tiled=True)
    gate = jnp.einsum("scd,df->scf", piece, gate_mat, preferred_element_type=jnp.float32)
    upward = jnp.einsum("scd,df->scf", piece, up_mat, preferred_element_type=jnp.float32)
    hidden = (jax.nn.silu(gate) * upward).astype(jnp.bfloat16)
    flat_hidden = hidden.reshape(-1, hidden.shape[2])
    summed = lax.psum_scatter(
        jnp.einsum("fd,sf->ds", down_mat, flat_hidden, preferred_element_type=jnp.float32).astype(
            jnp.bfloat16
        ),
        "tp",
        scatter_dimension=0,
        tiled=True,
    )
    back = lax.all_to_all(summed, "ep", split_axis=1, concat_axis=1, tiled=True)
    picked = (
        jnp.take(back, slot_index, axis=1).astype(jnp.float32).reshape(-1, row_count, top_count)
    )
    combined = jnp.einsum("drk,rk->rd", picked, route_weights)
    return combined.astype(jnp.bfloat16)


def visit_order(n):
    return [sorted((s for s in range(n) if s != e), key=lambda s: (abs(s - e), s)) for e in range(n)]


def fused_kernel(
    n,
    q_ref,
    k_ref,
    v_ref,
    lam_ref,
    hgain_ref,
    tok_ref,
    ids_ref,
    rw_ref,
    mgain_ref,
    wg_hbm,
    wu_hbm,
    wd_hbm,
    heads_ref,
    out_ref,
    wg,
    wu,
    wd,
    gathered,
    kbuf,
    vbuf,
    hid,
    part,
    core_in,
    s_own,
    s_out,
    x_in,
    t_out,
    ret,
    out_weights,
    wsem,
    own_send,
    z_send,
    z_recv,
    x_send,
    x_recv,
    c_send,
    c_recv,
    kv_send,
    kv_recv,
    r1_send,
    r1_recv,
    r2_send,
    r2_recv,
    r3_send,
    r3_recv,
):
    e = lax.axis_index("ep")
    t = lax.axis_index("tp")
    xi = t // 2
    ci = lax.rem(t, 2)
    core_peer = {"tp": 2 * xi + 1 - ci}
    x_peer = {"tp": 2 * (1 - xi) + ci}
    rows, width = tok_ref.shape
    cols = width // 4
    kv_rows = k_ref.shape[0]

    def colblock(j):
        return pl.ds(pl.multiple_of(j * cols, 128), cols)

    def remote(src, dst, ss, rs, dev):
        return pltpu.make_async_remote_copy(
            src_ref=src, dst_ref=dst, send_sem=ss, recv_sem=rs, device_id=dev, device_id_type=MESH
        )

    weights = [
        pltpu.make_async_copy(a, b, wsem.at[i])
        for i, (a, b) in enumerate(((wg_hbm.at[0], wg), (wu_hbm.at[0], wu), (wd_hbm.at[0], wd)))
    ]
    for c in weights:
        c.start()

    barrier = pltpu.get_barrier_semaphore()
    for d in range(1, n):
        pl.semaphore_signal(barrier, inc=1, device_id={"ep": lax.rem(e + d, n)}, device_id_type=MESH)
    pl.semaphore_signal(barrier, inc=1, device_id=core_peer, device_id_type=MESH)
    pl.semaphore_signal(barrier, inc=1, device_id=x_peer, device_id_type=MESH)

    halves = range(PIECES)
    hr = rows // PIECES

    def half(h):
        return pl.ds(h * hr, hr)

    def normalize(h):
        step = 32

        @pl.loop(0, hr // step)
        def _(i):
            sl = pl.ds(pl.multiple_of(h * hr + i * step, step), step)
            v = tok_ref[sl, :].astype(F32)
            scale = lax.rsqrt(jnp.mean(v * v, axis=1, keepdims=True) + 1e-06)
            gathered[e, sl, :] = (v * scale * mgain_ref[...]).astype(BF16)

    has_left = e > 0
    has_right = e < n - 1
    sides = ((0, has_left, e - 1), (1, has_right, e + 1))
    own_kv = pl.ds(pl.multiple_of(e * kv_rows, kv_rows), kv_rows)

    def own_tok(side, peer, h):
        blk = gathered.at[e, half(h), colblock(t)]
        return remote(blk, blk, own_send.at[side, h], z_recv.at[e, h], {"ep": peer})

    def kv_copies(s):
        dev = {"ep": s}
        return (
            remote(k_ref, kbuf.at[own_kv], kv_send.at[0, s], kv_recv.at[0, e], dev),
            remote(v_ref, vbuf.at[own_kv], kv_send.at[1, s], kv_recv.at[1, e], dev),
        )

    def kv_arrivals(s):
        sl = pl.ds(pl.multiple_of(s * kv_rows, kv_rows), kv_rows)
        return (
            remote(k_ref, kbuf.at[sl], kv_send.at[0, s], kv_recv.at[0, s], {"ep": s}),
            remote(v_ref, vbuf.at[sl], kv_send.at[1, s], kv_recv.at[1, s], {"ep": s}),
        )

    orders = visit_order(n)

    def nth(k):
        s = jnp.int32(orders[0][k])
        for i in range(1, n):
            s = jnp.where(e == i, jnp.int32(orders[i][k]), s)
        return s

    visits = [nth(k) for k in range(n - 1)]

    def forward_of(s):
        from_left = s < e
        has = jnp.logical_or(
            jnp.logical_and(from_left, has_right),
            jnp.logical_and(jnp.logical_not(from_left), has_left),
        )
        return has, {"ep": jnp.clip(jnp.where(from_left, e + 1, e - 1), 0, n - 1)}

    def z_copy(s, h):
        blk = gathered.at[s, half(h), colblock(t)]
        return remote(blk, blk, z_send.at[s, h], z_recv.at[s, h], forward_of(s)[1])

    def x_copy(s, h):
        blk = gathered.at[s, half(h), colblock(t)]
        return remote(blk, blk, x_send.at[s, h], x_recv.at[s, h], x_peer)

    def c_copy(s, h, which):
        blk = gathered.at[s, half(h), colblock(t if which == 0 else 2 * (1 - xi) + ci)]
        return remote(blk, blk, c_send.at[which, s, h], c_recv.at[which, s, h], core_peer)

    def r1_copy(s, h, xx):
        return remote(
            part.at[s, half(h), colblock(2 * xx + 1 - ci)],
            core_in.at[s, xx, half(h)],
            r1_send.at[xx, s, h],
            r1_recv.at[xx, s, h],
            core_peer,
        )

    def r2_copy(s, h):
        return remote(
            s_out.at[s, half(h)], x_in.at[s, half(h)], r2_send.at[s, h], r2_recv.at[s, h], x_peer
        )

    def r3_copy(s, h):
        return remote(
            t_out.at[s, half(h)],
            ret.at[e, half(h)],
            r3_send.at[s, h],
            r3_recv.at[e, h],
            {"ep": s},
        )

    ff = wg.shape[1]
    nb = ff // 3

    def up_step(s, b):
        sl = pl.ds(b * nb, nb)
        g = jnp.dot(gathered[s], wg[:, sl], preferred_element_type=F32)
        u = jnp.dot(gathered[s], wu[:, sl], preferred_element_type=F32)
        hid[:, sl] = (g / (1.0 + jnp.exp(-g)) * u).astype(BF16)

    def down_step(s, j):
        sl = colblock(j)
        part[s, :, sl] = jnp.dot(hid[...], wd[:, sl], preferred_element_type=F32).astype(BF16)

    def down(s):
        for xx in (1 - xi, xi):
            down_step(s, 2 * xx + 1 - ci)
            for h in halves:
                r1_copy(s, h, xx).start()
        for xx in (1 - xi, xi):
            down_step(s, 2 * xx + ci)

    def reduce_core(s):
        for h in halves:
            r1_copy(s, h, 1 - xi).wait_recv()
            s_out[s, half(h)] = (
                part[s, half(h), colblock(2 * (1 - xi) + ci)].astype(F32)
                + core_in[s, 1 - xi, half(h)].astype(F32)
            ).astype(BF16)
            r2_copy(s, h).start()
        for h in halves:
            r1_copy(s, h, xi).wait_recv()
        s_own[s] = part[s, :, colblock(t)].astype(F32) + core_in[s, xi].astype(F32)

    def reduce_x(s, send=True):
        for h in halves:
            r2_copy(s, h).wait_recv()
            t_out[s, half(h)] = (s_own[s, half(h)] + x_in[s, half(h)].astype(F32)).astype(BF16)
            if send:
                r3_copy(s, h).start()

    def take(s, h):
        z_copy(s, h).wait_recv()

        @pl.when(forward_of(s)[0])
        def _():
            z_copy(s, h).start()

    def share(s, h):
        x_copy(s, h).start()
        c_copy(s, h, 0).start()

    def arrive(s, h):
        take(s, h)
        share(s, h)

    def cross(s, h):
        x_copy(s, h).wait_recv()
        c_copy(s, h, 1).start()

    def ready(s):
        for h in halves:
            c_copy(s, h, 0).wait_recv()
            c_copy(s, h, 1).wait_recv()

    def attend(h):
        heads = lam_ref.shape[0]
        vd = v_ref.shape[1] // heads
        hd = q_ref.shape[1] // (2 * heads)
        qr = q_ref.shape[0]
        first = lax.broadcasted_iota(jnp.int32, (qr, 2 * hd), 1) < hd
        q = q_ref[:, h * 2 * hd : (h + 1) * 2 * hd].astype(F32)
        both = jnp.concatenate(
            [jnp.where(first, q, 0.0).astype(BF16), jnp.where(first, 0.0, q).astype(BF16)], axis=0
        )
        kh = kbuf[:, h * 2 * hd : (h + 1) * 2 * hd]
        vh = vbuf[:, h * vd : (h + 1) * vd]
        scores = lax.dot_general(
            both, kh, (((1,), (1,)), ((), ())), preferred_element_type=F32
        ) * (hd ** (-0.5))
        ex = jnp.exp(scores - jnp.max(scores, axis=1, keepdims=True))
        tot = jnp.sum(ex, axis=1, keepdims=True)
        sums = jnp.dot(ex.astype(BF16), vh, preferred_element_type=F32) / tot
        mixed = sums[:qr] - lam_ref[h] * sums[qr:]
        norm = lax.rsqrt(jnp.mean(mixed * mixed, axis=1, keepdims=True) + 1e-06)
        heads_ref[:, h * vd : (h + 1) * vd] = (mixed * norm * hgain_ref[...]).astype(BF16)

    for h in halves:
        normalize(h)
        if h == 0:
            pl.semaphore_wait(barrier, n + 1)
        for side, has, peer in sides:

            @pl.when(has)
            def _():
                own_tok(side, peer, h).start()

    kbuf[own_kv, :] = k_ref[...]
    vbuf[own_kv, :] = v_ref[...]

    def send_kv():
        for s in visits:
            for c in kv_copies(s):
                c.start()

    ids = ids_ref[...]
    rw = rw_ref[...]
    lines = [jnp.sum(jnp.where(ids == x, rw, 0.0), axis=0, keepdims=True) for x in [e] + visits]
    pad = (-len(lines)) % 8
    lines.append(jnp.zeros((pad, rows), F32))
    out_weights[...] = jnp.concatenate(lines, axis=0).T

    last = len(visits) - 1
    for c in weights:
        c.wait()
    for b in range(3):
        up_step(e, b)
    down(e)
    inner = jnp.logical_and(has_left, has_right)
    outer = jnp.logical_not(inner)

    @pl.when(inner)
    def _():
        for h in halves:
            arrive(visits[0], h)
            if last >= 1:
                take(visits[1], h)
        if last >= 1:
            for h in halves:
                share(visits[1], h)
        for h in halves:
            cross(visits[0], h)
        if last >= 2:
            for h in halves:
                arrive(visits[2], h)

    @pl.when(outer)
    def _():
        for h in halves:
            arrive(visits[0], h)
        for h in halves:
            cross(visits[0], h)
            if last >= 1:
                arrive(visits[1], h)

    ready(visits[0])
    for k, s in enumerate(visits):
        ahead = visits[k + 1] if k < last else None
        further = visits[k + 2] if k + 1 < last else None
        before = visits[k - 1] if k > 0 else None
        for b, group in enumerate((halves[: PIECES // 2], halves[PIECES // 2 :])):
            up_step(s, b)
            for h in group:
                if ahead is not None:
                    cross(ahead, h)
                if further is not None:
                    if k == 0:

                        @pl.when(outer)
                        def _():
                            arrive(further, h)

                    else:
                        arrive(further, h)
        if k == max(last - 2, 0):
            send_kv()
        if before is not None:
            reduce_core(before)
        up_step(s, 2)
        down(s)
        if ahead is not None:
            ready(ahead)
    for k in range(max(last - 1, 0)):
        reduce_x(visits[k])
    reduce_core(visits[last])
    reduce_core(e)
    heads = lam_ref.shape[0]
    for s in visits:
        for c in kv_arrivals(s):
            c.wait_recv()
    attend(0)
    if last >= 1:
        reduce_x(visits[last - 1])
    for h in range(1, heads):
        attend(h)
    reduce_x(visits[last])
    reduce_x(e, send=False)

    total = out_weights[:, 0:1] * t_out[e].astype(F32)
    for k, s in enumerate(visits):
        for h in halves:
            remote(
                t_out.at[s, half(h)],
                ret.at[s, half(h)],
                r3_send.at[s, h],
                r3_recv.at[s, h],
                {"ep": s},
            ).wait_recv()
        total = total + ret[s].astype(F32) * out_weights[:, k + 1 : k + 2]
    out_ref[...] = total.astype(BF16)

    for side, has, peer in sides:

        @pl.when(has)
        def _():
            for h in halves:
                own_tok(side, peer, h).wait_send()

    for s in [e] + visits:
        for h in halves:
            r1_copy(s, h, 1 - xi).wait_send()
            r1_copy(s, h, xi).wait_send()
            r2_copy(s, h).wait_send()
    for s in visits:
        for h in halves:
            x_copy(s, h).wait_send()
            c_copy(s, h, 0).wait_send()
            c_copy(s, h, 1).wait_send()
            r3_copy(s, h).wait_send()
        for c in kv_copies(s):
            c.wait_send()

        @pl.when(forward_of(s)[0])
        def _():
            for h in halves:
                z_copy(s, h).wait_send()


def hand_on_kernel(a_ref, b_ref, c_ref, d_ref):
    c_ref[...] = a_ref[...]
    d_ref[...] = b_ref[...]


def fused(queries, keys, values, lambdas, head_gain, tokens, route_ids, route_weights, moe_gain, w_gate, w_up, w_down):
    n = lax.axis_size("ep")
    rows, width = tokens.shape
    cols = width // 4
    ff = w_gate.shape[2]
    vmem = pl.BlockSpec(memory_space=pltpu.VMEM)
    smem = pl.BlockSpec(memory_space=pltpu.SMEM)
    hbm = pl.BlockSpec(memory_space=pl.ANY)
    dma = pltpu.SemaphoreType.DMA
    results = pl.pallas_call(
        functools.partial(fused_kernel, n),
        out_shape=(
            jax.ShapeDtypeStruct((queries.shape[0], values.shape[1]), BF16),
            jax.ShapeDtypeStruct((rows, cols), BF16),
        ),
        in_specs=[vmem, vmem, vmem, smem, vmem, vmem, vmem, vmem, vmem, hbm, hbm, hbm],
        out_specs=(vmem, vmem),
        scratch_shapes=[
            pltpu.VMEM((width, ff), BF16),
            pltpu.VMEM((width, ff), BF16),
            pltpu.VMEM((ff, width), BF16),
            pltpu.VMEM((n, rows, width), BF16),
            pltpu.VMEM((n * keys.shape[0], keys.shape[1]), BF16),
            pltpu.VMEM((n * values.shape[0], values.shape[1]), BF16),
            pltpu.VMEM((rows, ff), BF16),
            pltpu.VMEM((n, rows, width), BF16),
            pltpu.VMEM((n, 2, rows, cols), BF16),
            pltpu.VMEM((n, rows, cols), F32),
            pltpu.VMEM((n, rows, cols), BF16),
            pltpu.VMEM((n, rows, cols), BF16),
            pltpu.VMEM((n, rows, cols), BF16),
            pltpu.VMEM((n, rows, cols), BF16),
            pltpu.VMEM((rows, -(-n // 8) * 8), F32),
            dma((3,)),
            dma((2, PIECES)),
            dma((n, PIECES)),
            dma((n, PIECES)),
            dma((n, PIECES)),
            dma((n, PIECES)),
            dma((2, n, PIECES)),
            dma((2, n, PIECES)),
            dma((2, n)),
            dma((2, n)),
            dma((2, n, PIECES)),
            dma((2, n, PIECES)),
            dma((n, PIECES)),
            dma((n, PIECES)),
            dma((n, PIECES)),
            dma((n, PIECES)),
        ],
        compiler_params=pltpu.CompilerParams(
            collective_id=0, has_side_effects=True, vmem_limit_bytes=60 * 1024 * 1024
        ),
        name="fused_layer",
    )(
        queries,
        keys,
        values,
        lambdas,
        head_gain,
        tokens,
        route_ids.T,
        route_weights.T,
        moe_gain,
        w_gate,
        w_up,
        w_down,
    )
    return pl.pallas_call(
        hand_on_kernel,
        out_shape=tuple(jax.ShapeDtypeStruct(r.shape, r.dtype) for r in results),
        in_specs=[vmem, vmem],
        out_specs=(vmem, vmem),
        name="hand_on",
    )(*results)


def on_device(
    queries,
    keys,
    values,
    lambdas,
    head_gain,
    tokens,
    route_ids,
    route_weights,
    moe_gain,
    w_gate,
    w_up,
    w_down,
):
    rows = tokens.shape[0]
    expert_count = w_gate.shape[0] * lax.axis_size("ep")
    slots = 2 * rows * route_ids.shape[1] // expert_count
    if w_gate.shape[0] == 1 and lax.axis_size("tp") == 4 and slots >= rows:
        return fused(
            queries, keys, values, lambdas, head_gain, tokens,
            route_ids, route_weights, moe_gain, w_gate, w_up, w_down,
        )
    heads_out = attend(queries, keys, values, lambdas, head_gain)
    expert_out = experts(tokens, route_ids, route_weights, moe_gain, w_gate, w_up, w_down)
    return (heads_out, expert_out)


def solution(mesh):
    in_specs = (
        P(("grp", "ep"), "tp"),
        P(("grp", "ep"), "tp"),
        P(("grp", "ep"), "tp"),
        P("tp"),
        P(),
        P(("grp", "ep"), None),
        P(("grp", "ep"), None),
        P(("grp", "ep"), None),
        P(),
        P("ep", None, "tp"),
        P("ep", None, "tp"),
        P("ep", "tp", None),
    )
    out_specs = (P(("grp", "ep"), "tp"), P(("grp", "ep"), "tp"))
    return jax.shard_map(
        on_device, mesh=mesh, in_specs=in_specs, out_specs=out_specs, check_vma=False
    )
```
